32 devices in a mesh: grp: 2 (over y), sp: 4 (over z), tp: 4 (over x, core).
Axes of the slice: x: 2, y: 2, z: 4, core: 2. Of those that a mesh axis runs over, the one named last changes fastest.
Arguments:
- queries: bfloat16 [1024, 512], P(('grp', 'sp'), 'tp'), parts along dimension 0, may hold values from -6 to 6
- key_rows: bfloat16 [1024, 512], P(('grp', 'sp'), 'tp'), parts along dimension 0, may hold values from -6 to 6
- value_rows: bfloat16 [1024, 512], P(('grp', 'sp'), 'tp'), parts along dimension 0, may hold values from -16 to 16
- key_bias: bfloat16 [8, 1024], P('tp', ('grp', 'sp')), parts along dimension 1, may hold values from -20 to 0
- residual: bfloat16 [1024, 2048], P(('grp', 'sp')), parts along dimension 0, may hold values from -6 to 6
- out_weight: bfloat16 [512, 2048], P('tp'), may hold values from -0.25 to 0.25
- norm_gain: bfloat16 [2048], replicated, may hold values from 0.099609375 to 1.8984375
- gate_weight: bfloat16 [2048, 3072], P('sp', 'tp'), may hold values from -0.125 to 0.125
- up_weight: bfloat16 [2048, 3072], P('sp', 'tp'), may hold values from -0.125 to 0.125
- down_weight: bfloat16 [3072, 2048], P('tp', 'sp'), may hold values from -0.109375 to 0.109375
Outputs:
- layer_out: bfloat16 [1024, 2048], P(('grp', 'sp')), parts along dimension 0
The draws below stay inside these ranges and needn't reach their ends.
There are 2 independent parts, one for each index of `grp`. The reference program is written for one: setup_inputs(seed, part) draws one part's arguments, and reference() takes and returns one part's arrays. A program takes and returns all parts, laid end to end along the dimension named above; an argument that names none is the same for every part. Nothing has to cross between parts.
All inputs are finite; a program needn't handle non-finite values.
Results may differ from the reference program's by a relative error of at most 0.014.
Values may be sent and summed in bfloat16 or wider, within the bound.
A program may use at most 64 MiB of HBM per device.

```python
import jax
import jax.numpy as jnp
from jax import lax

D = 2048
HEAD_TOTAL = 8
HEAD_DIM = 64
FF = 3072
TOK_DEV = 128
SEQUENCE_LENGTH = 512
QK = 512
N_TP = 4


def draw_value_rows(key, part):
    first_key, second_key = jax.random.split(jax.random.fold_in(key, 11))
    span_len = max(TOK_DEV // 2, 1)
    n_spans = SEQUENCE_LENGTH // span_len
    offsets = 2.0 * jax.random.normal(first_key, (n_spans, 1, QK), jnp.float32)
    noise = jax.random.normal(second_key, (n_spans, span_len, QK), jnp.float32)
    return jnp.clip((offsets + noise).reshape(SEQUENCE_LENGTH, QK), -16.0, 16.0).astype(jnp.bfloat16)


def draw_key_bias(key, part):
    random_subkey_list = jax.random.split(jax.random.fold_in(key, 23), 6)
    span_len = max(TOK_DEV // 2, 1)
    n_spans = SEQUENCE_LENGTH // span_len
    share = 0.5
    fast = jax.random.uniform(random_subkey_list[0], (HEAD_TOTAL, 1, 1), jnp.float32) < share
    slow_level = -jnp.log(SEQUENCE_LENGTH * 1.0) - 1.0 + jax.random.uniform(random_subkey_list[1], (HEAD_TOTAL, 1, 1), jnp.float32, minval=-0.5, maxval=0.5)
    fast_level = -3.7 + jax.random.uniform(random_subkey_list[2], (HEAD_TOTAL, 1, 1), jnp.float32, minval=-0.5, maxval=0.5)
    level = jnp.where(fast, fast_level, slow_level)
    factor = jax.random.uniform(random_subkey_list[3], (HEAD_TOTAL, n_spans, 1), jnp.float32, minval=-0.9, maxval=0.9)
    smoothed_values = (level + factor + jnp.zeros((HEAD_TOTAL, n_spans, span_len), jnp.float32)).reshape(HEAD_TOTAL, SEQUENCE_LENGTH)
    spike_amount = jax.random.uniform(random_subkey_list[4], (HEAD_TOTAL, SEQUENCE_LENGTH), jnp.float32) < 3.0 / SEQUENCE_LENGTH
    spike_threshold = jax.random.uniform(random_subkey_list[5], (HEAD_TOTAL, SEQUENCE_LENGTH), jnp.float32, minval=-1.0, maxval=0.0)
    return jnp.where(spike_amount, spike_threshold, smoothed_values).astype(jnp.bfloat16)


def shard_levels(key, extent, cuts, least, top_value):
    def one(position, parts):
        steps = jax.random.uniform(jax.random.fold_in(jax.random.fold_in(key, 6), position), (parts,), jnp.float32, least / len(cuts), top_value / len(cuts))
        return jnp.repeat(jnp.exp(steps), extent[position] // parts).reshape((-1,) + (1,) * (len(extent) - position - 1))

    factor_of = one(*cuts[0])
    for cut in cuts[1:]:
        factor_of = factor_of * one(*cut)
    return factor_of


def gaussian(rng, shape, spread, reach, cuts=(), kind=jnp.bfloat16):
    factor_of = shard_levels(rng, shape, cuts, -0.22, 0.18) if cuts else 1.0
    drawn = jax.random.normal(rng, shape, jnp.float32) * spread * factor_of
    return jnp.minimum(jnp.maximum(drawn, -reach), reach).astype(kind)


def setup_inputs(seed: int = 0, part: int = 0) -> dict:
    key_list = jax.random.split(jax.random.key(seed), 11)
    part_keys = jax.random.split(jax.random.fold_in(key_list[10], part), 11)
    return {
        "queries": gaussian(part_keys[0], (SEQUENCE_LENGTH, QK), 1.0, 6.0, ((0, 4), (1, 4))),
        "key_rows": gaussian(part_keys[1], (SEQUENCE_LENGTH, QK), 1.0, 6.0, ((0, 4), (1, 4))),
        "value_rows": draw_value_rows(jax.random.fold_in(jax.random.fold_in(key_list[10], part), 71), part),
        "key_bias": draw_key_bias(jax.random.fold_in(jax.random.fold_in(key_list[10], part), 71), part),
        "residual": gaussian(part_keys[4], (SEQUENCE_LENGTH, D), 1.0, 6.0, ((0, 4),)),
        "out_weight": gaussian(key_list[5], (QK, D), QK ** -0.5, 0.25, ((0, 4),)),
        "norm_gain": jnp.clip(1.0 + 0.18 * jax.random.normal(key_list[6], (D,), jnp.float32), 0.099609375, 1.8984375).astype(jnp.bfloat16),
        "gate_weight": gaussian(key_list[7], (D, FF), D ** -0.5, 0.125, ((0, 4), (1, 4))),
        "up_weight": gaussian(key_list[8], (D, FF), D ** -0.5, 0.125, ((0, 4), (1, 4))),
        "down_weight": gaussian(key_list[9], (FF, D), FF ** -0.5, 0.109375, ((0, 4), (1, 4))),
    }


def stick_attention(queries, key_rows, value_rows, key_bias):
    query_heads = queries.reshape(SEQUENCE_LENGTH, HEAD_TOTAL, HEAD_DIM).astype(jnp.float32)
    key_heads = key_rows.reshape(SEQUENCE_LENGTH, HEAD_TOTAL, HEAD_DIM).astype(jnp.float32)
    value_heads = value_rows.reshape(SEQUENCE_LENGTH, HEAD_TOTAL, HEAD_DIM).astype(jnp.float32)
    bias_all = key_bias.astype(jnp.float32)
    key_pos = lax.iota(jnp.int32, SEQUENCE_LENGTH)

    def one_block(block_index):
        begin = (block_index * TOK_DEV).astype(jnp.int32)
        query_block = lax.dynamic_slice_in_dim(query_heads, begin, TOK_DEV, 0)
        scores = jnp.einsum('qhd,khd->hqk', query_block, key_heads) * HEAD_DIM ** (-0.5)
        scores = scores + bias_all[:, None, :]
        query_pos = begin + lax.iota(jnp.int32, TOK_DEV)
        strict = (key_pos[None, :] < query_pos[:, None])[None]
        log_retained = jnp.where(strict, jax.nn.log_sigmoid(-scores), 0.0)
        between = lax.cumsum(log_retained, axis=2, reverse=True) - log_retained
        stick = jnp.where(strict, jnp.exp(jax.nn.log_sigmoid(scores) + between), 0.0).astype(jnp.bfloat16)
        stick = lax.optimization_barrier(stick).astype(jnp.float32)
        return jnp.einsum('hqk,khd->qhd', stick, value_heads)
    blocks = lax.map(one_block, jnp.arange(SEQUENCE_LENGTH // TOK_DEV, dtype=jnp.int32))
    return blocks.reshape(SEQUENCE_LENGTH, QK).astype(jnp.bfloat16)

def grouped_product(left, right, groups):
    width_group = left.shape[1] // groups
    summed = jnp.zeros((left.shape[0], right.shape[1]), jnp.float32)
    for group in range(groups):
        part_prod = jnp.dot(left[:, group * width_group:(group + 1) * width_group], right[group * width_group:(group + 1) * width_group], preferred_element_type=jnp.float32).astype(jnp.bfloat16)
        summed = summed + lax.optimization_barrier(part_prod).astype(jnp.float32)
    return summed

def reference(queries, key_rows, value_rows, key_bias, residual, out_weight, norm_gain, gate_weight, up_weight, down_weight):
    attended = stick_attention(queries, key_rows, value_rows, key_bias)
    mixed = grouped_product(attended, out_weight, N_TP)
    middle = (residual.astype(jnp.float32) + mixed).astype(jnp.bfloat16)
    middle_wide = lax.optimization_barrier(middle).astype(jnp.float32)
    mean_square = lax.optimization_barrier(jnp.mean(middle_wide * middle_wide, axis=1, keepdims=True))
    normed = (middle_wide * lax.rsqrt(mean_square + 1e-05) * norm_gain.astype(jnp.float32)).astype(jnp.bfloat16)
    gate_pre = jnp.dot(normed, gate_weight, preferred_element_type=jnp.float32)
    up_pre = jnp.dot(normed, up_weight, preferred_element_type=jnp.float32)
    hidden = (jax.nn.silu(gate_pre) * up_pre).astype(jnp.bfloat16)
    down_sum = grouped_product(hidden, down_weight, N_TP)
    return (middle_wide + down_sum).astype(jnp.bfloat16)
```

```python
import functools

import jax
import jax.numpy as jnp
from jax import lax
from jax.experimental import pallas as pl
from jax.experimental.pallas import tpu as pltpu
from jax.sharding import PartitionSpec as P

norm_eps = 1e-05


def from_behind(value, axis, steps):
    count = lax.axis_size(axis)
    initial, last = (max(0, -steps), min(count, count - steps))
    return lax.ppermute(value, axis, [(source, source + steps) for source in range(initial, last)])


def stick_block(carry, query_heads, key_block, value_block, bias_block, query_pos, key_start):
    accum, kept_log = carry
    key_count = key_block.shape[0]
    head_count = query_heads.shape[1]
    key_heads = key_block.reshape(key_count, head_count, -1)
    value_heads = value_block.reshape(key_count, head_count, -1)
    scale = key_heads.shape[2] ** (-0.5)
    scores = (
        jnp.einsum("qhd,khd->hqk", query_heads, key_heads, preferred_element_type=jnp.float32)
        * scale
    )
    scores = scores + bias_block.astype(jnp.float32)[:, None, :]
    key_pos = key_start + lax.iota(jnp.int32, key_count)
    strict = ((key_pos[None, :] < query_pos[:, None]) & (key_pos[None, :] >= 0))[None]
    log_retained = jnp.where(strict, jax.nn.log_sigmoid(-scores), 0.0)
    between = lax.cumsum(log_retained, axis=2, reverse=True) - log_retained + kept_log[:, :, None]
    stick = jnp.where(strict, jnp.exp(jax.nn.log_sigmoid(scores) + between), 0.0).astype(
        jnp.bfloat16
    )
    accum = accum + jnp.einsum(
        "hqk,khd->qhd", stick, value_heads, preferred_element_type=jnp.float32
    )
    return (accum, kept_log + jnp.sum(log_retained, axis=2))


def normalize(middle_wide, norm_gain):
    mean_square = jnp.mean(middle_wide * middle_wide, axis=1, keepdims=True)
    return (middle_wide * lax.rsqrt(mean_square + norm_eps) * norm_gain.astype(jnp.float32)).astype(
        jnp.bfloat16
    )


def body(
    queries,
    key_rows,
    value_rows,
    key_bias,
    residual,
    out_weight,
    norm_gain,
    gate_weight,
    up_weight,
    down_weight,
):
    seg_rows = queries.shape[0]
    head_count = key_bias.shape[0]
    head_width = queries.shape[1] // head_count
    sp_count = lax.axis_size("sp")
    token_place = lax.axis_index("sp")
    query_heads = queries.reshape(seg_rows, head_count, head_width)
    query_pos = token_place * seg_rows + lax.iota(jnp.int32, seg_rows)
    start_carry = (
        jnp.zeros((seg_rows, head_count, head_width), jnp.float32),
        jnp.zeros((head_count, seg_rows), jnp.float32),
    )
    carry = stick_block(
        start_carry, query_heads, key_rows, value_rows, key_bias, query_pos, token_place * seg_rows
    )

    def advance(hop_index, state):
        carry_now, blocks = state
        blocks = from_behind((blocks[0], blocks[1], blocks[2]), "sp", 1)

        def attend(current):
            return stick_block(
                current,
                query_heads,
                blocks[0],
                blocks[1],
                blocks[2],
                query_pos,
                (token_place - hop_index) * seg_rows,
            )

        carry_now = lax.cond(token_place >= hop_index, attend, lambda current: current, carry_now)
        return (carry_now, blocks)

    carry, passed_blocks = lax.fori_loop(
        1, sp_count, advance, (carry, (key_rows, value_rows, key_bias))
    )
    attended = carry[0].reshape(seg_rows, head_count * head_width).astype(jnp.bfloat16)
    own_rows = seg_rows // lax.axis_size("tp")
    own_start = lax.axis_index("tp") * own_rows
    mixed = lax.psum_scatter(
        jnp.dot(attended, out_weight, preferred_element_type=jnp.float32).astype(jnp.bfloat16),
        "tp",
        scatter_dimension=0,
        tiled=True,
    ).astype(jnp.float32)
    own_residual = lax.dynamic_slice_in_dim(residual, own_start, own_rows, 0)
    middle = (own_residual.astype(jnp.float32) + mixed).astype(jnp.bfloat16)
    middle_wide = middle.astype(jnp.float32)
    normed_all = lax.all_gather(normalize(middle_wide, norm_gain), "tp", axis=0, tiled=True)
    gate_pre = jnp.dot(
        normed_all,
        lax.all_gather(gate_weight, "sp", axis=0, tiled=True),
        preferred_element_type=jnp.float32,
    )
    up_pre = jnp.dot(
        normed_all,
        lax.all_gather(up_weight, "sp", axis=0, tiled=True),
        preferred_element_type=jnp.float32,
    )
    hidden = (jax.nn.silu(gate_pre) * up_pre).astype(jnp.bfloat16)
    down_terms = jnp.dot(
        hidden,
        lax.all_gather(down_weight, "sp", axis=1, tiled=True),
        preferred_element_type=jnp.float32,
    )
    down_sum = lax.psum_scatter(
        down_terms.astype(jnp.bfloat16), "tp", scatter_dimension=0, tiled=True
    ).astype(jnp.float32)
    own_out = (middle_wide + down_sum).astype(jnp.bfloat16)
    return lax.all_gather(own_out, "tp", axis=0, tiled=True)


def contract(left, right, dims):
    return lax.dot_general(left, right, ((dims[:1], dims[1:]), ((), ())), preferred_element_type=jnp.float32)


def layer_kernel(
    grp_count,
    sp_count,
    tp_count,
    q_ref,
    k_ref,
    v_ref,
    bias_ref,
    res_ref,
    ow_ref,
    gain_ref,
    gate_ref,
    up_ref,
    down_ref,
    out_ref,
    kbuf,
    vbuf,
    bbuf,
    acc,
    kept,
    wsend,
    w_all,
    pbuf,
    rbuf,
    middle,
    n_all,
    h_all,
    dbuf,
    rdown,
    zsend,
    zin,
    kv_sems,
    w_sems,
    wy_sems,
    r_sems,
    n_sems,
    f_sems,
    h_sems,
    d_sems,
    z_sems,
    o_sems,
):
    g, s, t = lax.axis_index("grp"), lax.axis_index("sp"), lax.axis_index("tp")
    rows, model = res_ref.shape
    quarter = rows // tp_count
    slab = model // sp_count
    piece = gate_ref.shape[1] // sp_count
    head_count = bias_ref.shape[0]
    width = q_ref.shape[1] // head_count
    sends = []

    def sp_peer(step):
        return lax.rem(s + step + sp_count, sp_count)

    def tp_peer(step):
        return lax.rem(t + step + tp_count, tp_count)

    core_mate = t + 1 - 2 * lax.rem(t, 2)
    far_mate = lax.rem(t + 2, 4)

    def copy(source, target, sems, index, device):
        return pltpu.make_async_remote_copy(
            src_ref=source,
            dst_ref=target,
            send_sem=sems.at[(0,) + index],
            recv_sem=sems.at[(1,) + index],
            device_id=device,
            device_id_type=pl.DeviceIdType.MESH,
        )

    def launch(*arguments):
        made = copy(*arguments)
        made.start()
        sends.append(made)
        return made

    barrier = pltpu.get_barrier_semaphore()
    for step in range(1, sp_count):
        pl.semaphore_signal(barrier, inc=1, device_id=(g, sp_peer(step), t), device_id_type=pl.DeviceIdType.MESH)
    for step in range(1, tp_count):
        pl.semaphore_signal(barrier, inc=1, device_id=(g, s, tp_peer(step)), device_id_type=pl.DeviceIdType.MESH)
    pl.semaphore_signal(barrier, inc=1, device_id=(1 - g, s, t), device_id_type=pl.DeviceIdType.MESH)
    pl.semaphore_wait(barrier, sp_count + tp_count - 1)

    kv_copies = {}
    for step in range(1, sp_count):
        device = (g, sp_peer(step), t)
        kv_copies[step] = [
            copy(k_ref, kbuf.at[step - 1], kv_sems, (0, step - 1), device),
            copy(v_ref, vbuf.at[step - 1], kv_sems, (1, step - 1), device),
            copy(bias_ref, bbuf.at[step - 1], kv_sems, (2, step - 1), device),
        ]

        @pl.when(s + step < sp_count)
        def _():
            for made in kv_copies[step]:
                made.start()

    for part, ref in ((0, gate_ref), (1, up_ref)):
        for start in range(0, ref.shape[1], 128):
            wsend[part, start : start + 128, :] = ref[:, start : start + 128].T
    w_copies = {}
    for step in range(1, sp_count):
        dest = sp_peer(step)
        w_copies[step] = launch(
            wsend.at[g, pl.ds(pl.multiple_of(dest * piece, 16), piece)],
            w_all.at[s, g],
            w_sems,
            (step - 1,),
            (g, dest, t),
        )
    for part in range(2):
        w_all[s, part] = wsend[part, pl.ds(pl.multiple_of(s * piece, 16), piece), :]

    acc[...] = jnp.zeros_like(acc)
    kept[...] = jnp.zeros_like(kept)
    query = q_ref[...]
    lane = lax.broadcasted_iota(jnp.int32, query.shape, 1)
    row_id = lax.broadcasted_iota(jnp.int32, (rows, rows), 0)
    col_id = lax.broadcasted_iota(jnp.int32, (rows, rows), 1)
    later = (row_id > col_id).astype(jnp.bfloat16)
    scale = width ** (-0.5)

    def attend(key_block, value_block, bias_block, diagonal):
        bias_wide = bias_block.astype(jnp.float32)
        for head in range(head_count):
            mine = (lane >= head * width) & (lane < (head + 1) * width)
            zero = jnp.zeros_like(query)
            scores = contract(jnp.where(mine, query, zero), key_block, (1, 1)) * scale
            scores = scores + bias_wide[head : head + 1, :]
            soft = jnp.log1p(jnp.exp(-jnp.abs(scores)))
            log_take = jnp.minimum(scores, 0.0) - soft
            log_keep = -jnp.maximum(scores, 0.0) - soft
            if diagonal:
                log_keep = jnp.where(col_id < row_id, log_keep, 0.0)
            high = log_keep.astype(jnp.bfloat16)
            low = (log_keep - high.astype(jnp.float32)).astype(jnp.bfloat16)
            between = contract(high, later, (1, 0)) + contract(low, later, (1, 0)) + kept[head]
            stick = jnp.exp(log_take + between)
            if diagonal:
                stick = jnp.where(col_id < row_id, stick, 0.0)
            acc[...] += contract(
                stick.astype(jnp.bfloat16), jnp.where(mine, value_block, zero), (1, 0)
            )
            kept[head] = kept[head] + jnp.sum(log_keep, axis=1, keepdims=True)

    attend(k_ref[...], v_ref[...], bias_ref[...], True)
    for step in range(1, sp_count):

        @pl.when(s >= step)
        def _():
            for made in kv_copies[step]:
                made.wait_recv()
            attend(kbuf[step - 1], vbuf[step - 1], bbuf[step - 1], False)

    attended = acc[...].astype(jnp.bfloat16)
    for start in range(0, model, 512):
        pbuf[:, start : start + 512] = contract(
            attended, ow_ref[:, start : start + 512], (1, 0)
        ).astype(jnp.bfloat16)

    def own_rows(index):
        return pl.ds(pl.multiple_of(index * quarter, quarter), quarter)

    r_copies = []
    for step in range(1, tp_count):
        dest = tp_peer(step)
        r_copies.append(
            launch(pbuf.at[own_rows(dest)], rbuf.at[step - 1], r_sems, (step - 1,), (g, s, dest))
        )
    mixed = pbuf[own_rows(t), :].astype(jnp.float32)
    for index, made in enumerate(r_copies):
        made.wait_recv()
        mixed = mixed + rbuf[index].astype(jnp.float32)
    middle[...] = (res_ref[own_rows(t), :].astype(jnp.float32) + mixed).astype(jnp.bfloat16)
    wide = middle[...].astype(jnp.float32)
    mean_square = jnp.mean(wide * wide, axis=1, keepdims=True)
    n_all[s, t] = (
        wide * lax.rsqrt(mean_square + norm_eps) * gain_ref[...].astype(jnp.float32)
    ).astype(jnp.bfloat16)

    n_copies = {}
    for step in range(1, sp_count):
        n_copies[step] = launch(
            n_all.at[s, t], n_all.at[s, t], n_sems, (step - 1,), (g, sp_peer(step), t)
        )

    def spread(ref, sems, index):
        return (
            launch(ref(t), ref(t), sems, (0, index), (g, s, far_mate)),
            launch(ref(t), ref(t), sems, (1, index), (g, s, core_mate)),
        )

    def finish(ref, sems, index, first):
        first[0].wait_recv()
        relayed = launch(ref(far_mate), ref(far_mate), sems, (2, index), (g, s, core_mate))
        first[1].wait_recv()
        relayed.wait_recv()

    def n_view(block):
        return lambda place: n_all.at[block, place]

    spreads = {0: spread(n_view(s), f_sems, 0)}
    y_copies = []
    for step in range(1, sp_count):
        w_copies[step].wait_recv()
        view = w_all.at[sp_peer(-step), g]
        y_copies.append(launch(view, view, wy_sems, (step - 1,), (1 - g, s, t)))
    for step in range(1, sp_count):
        n_copies[step].wait_recv()
        spreads[step] = spread(n_view(sp_peer(-step)), f_sems, step)
    for made in y_copies:
        made.wait_recv()

    h_copies = {}
    for step in range(sp_count):
        block = sp_peer(-step)
        finish(n_view(block), f_sems, step, spreads[step])
        total = jnp.zeros((2 * piece, rows), jnp.float32)
        tokens = n_all[block].reshape(rows, model)
        for part in range(sp_count):
            total = total + contract(
                w_all[part].reshape(2 * piece, slab),
                tokens[:, part * slab : (part + 1) * slab],
                (1, 1),
            )
        gate_pre, up_pre = total[:piece], total[piece:]
        h_all[block, s] = (gate_pre / (1.0 + jnp.exp(-gate_pre)) * up_pre).astype(jnp.bfloat16)
        for hop in range(1, sp_count):
            h_copies[step, hop] = launch(
                h_all.at[block, s], h_all.at[block, s], h_sems, (step, hop - 1), (g, sp_peer(hop), t)
            )

    d_copies = {}
    order = list(range(1, sp_count)) + [0]
    for step in order:
        block = sp_peer(-step)
        for hop in range(1, sp_count):
            h_copies[(step - hop) % sp_count, hop].wait_recv()
        hidden = h_all[block].reshape(sp_count * piece, rows)
        dbuf[block] = contract(hidden, down_ref[...], (0, 0)).astype(jnp.bfloat16)
        for hop in range(1, tp_count):
            dest = tp_peer(hop)
            d_copies[step, hop] = launch(
                dbuf.at[block, own_rows(dest)],
                rdown.at[hop - 1, step],
                d_sems,
                (step, hop - 1),
                (g, s, dest),
            )
    z_copies = {}
    for step in order:
        block = sp_peer(-step)
        summed = dbuf[block, own_rows(t), :].astype(jnp.float32)
        for hop in range(1, tp_count):
            d_copies[step, hop].wait_recv()
            summed = summed + rdown[hop - 1, step].astype(jnp.float32)
        if step:
            zsend[step - 1] = summed.astype(jnp.bfloat16)
            z_copies[step] = launch(
                zsend.at[step - 1], zin.at[s], z_sems, (step - 1,), (g, block, t)
            )
        else:
            zin[s] = summed.astype(jnp.bfloat16)
    for step in range(1, sp_count):
        z_copies[step].wait_recv()
    for part in range(sp_count):
        cols = slice(part * slab, (part + 1) * slab)
        out_ref[own_rows(t), cols] = (
            middle[:, cols].astype(jnp.float32) + zin[part].astype(jnp.float32)
        ).astype(jnp.bfloat16)

    def out_view(place):
        return out_ref.at[own_rows(place)]

    finish(out_view, o_sems, 0, spread(out_view, o_sems, 0))
    for made in sends:
        made.wait_send()
    for step in range(1, sp_count):

        @pl.when(s + step < sp_count)
        def _():
            for made in kv_copies[step]:
                made.wait_send()


def fused_body(
    grp_count,
    sp_count,
    tp_count,
    queries,
    key_rows,
    value_rows,
    key_bias,
    residual,
    out_weight,
    norm_gain,
    gate_weight,
    up_weight,
    down_weight,
):
    rows, columns = queries.shape
    head_count = key_bias.shape[0]
    model = residual.shape[1]
    hidden = gate_weight.shape[1]
    piece, slab, quarter = hidden // sp_count, model // sp_count, rows // tp_count
    n, m = sp_count - 1, tp_count - 1
    half, wide = jnp.bfloat16, jnp.float32
    dma = pltpu.SemaphoreType.DMA
    return pl.pallas_call(
        functools.partial(layer_kernel, grp_count, sp_count, tp_count),
        out_shape=jax.ShapeDtypeStruct((rows, model), half),
        in_specs=[pl.BlockSpec(memory_space=pltpu.VMEM)] * 10,
        out_specs=pl.BlockSpec(memory_space=pltpu.VMEM),
        scratch_shapes=[
            pltpu.VMEM((n, rows, columns), half),
            pltpu.VMEM((n, rows, columns), half),
            pltpu.VMEM((n, head_count, rows), half),
            pltpu.VMEM((rows, columns), wide),
            pltpu.VMEM((head_count, rows, 1), wide),
            pltpu.VMEM((2, hidden, slab), half),
            pltpu.VMEM((sp_count, 2, piece, slab), half),
            pltpu.VMEM((rows, model), half),
            pltpu.VMEM((m, quarter, model), half),
            pltpu.VMEM((quarter, model), half),
            pltpu.VMEM((sp_count, tp_count, quarter, model), half),
            pltpu.VMEM((sp_count, sp_count, piece, rows), half),
            pltpu.VMEM((sp_count, rows, slab), half),
            pltpu.VMEM((m, sp_count, quarter, slab), half),
            pltpu.VMEM((n, quarter, slab), half),
            pltpu.VMEM((sp_count, quarter, slab), half),
            dma((2, 3, n)),
            dma((2, n)),
            dma((2, n)),
            dma((2, m)),
            dma((2, n)),
            dma((2, 3, sp_count)),
            dma((2, sp_count, n)),
            dma((2, sp_count, m)),
            dma((2, n)),
            dma((2, 3, 1)),
        ],
        compiler_params=pltpu.CompilerParams(
            collective_id=0, has_side_effects=True, vmem_limit_bytes=48 * 1024 * 1024
        ),
    )(
        queries,
        key_rows,
        value_rows,
        key_bias,
        residual,
        out_weight,
        norm_gain.reshape(1, model),
        gate_weight,
        up_weight,
        down_weight,
    )


def any_body(sizes, *arguments):
    grp_count, sp_count, tp_count = sizes
    queries, model, hidden = arguments[0], arguments[4].shape[1], arguments[7].shape[1]
    rows = queries.shape[0]
    fits = (
        grp_count == 2
        and tp_count == 4
        and 1 < sp_count <= 4
        and rows == 128
        and queries.shape[1] == 128
        and (model // sp_count) % 128 == 0
        and (hidden // sp_count) % 16 == 0
        and hidden % 128 == 0
    )
    if fits:
        return fused_body(grp_count, sp_count, tp_count, *arguments)
    return body(*arguments)


def solution(mesh):
    in_specs = (
        P(("grp", "sp"), "tp"),
        P(("grp", "sp"), "tp"),
        P(("grp", "sp"), "tp"),
        P("tp", ("grp", "sp")),
        P(("grp", "sp"), None),
        P("tp", None),
        P(),
        P("sp", "tp"),
        P("sp", "tp"),
        P("tp", "sp"),
    )
    out_specs = P(("grp", "sp"), None)
    sizes = tuple(mesh.shape[name] for name in ("grp", "sp", "tp"))
    return jax.shard_map(functools.partial(any_body, sizes), mesh=mesh, in_specs=in_specs, out_specs=out_specs, check_vma=False)
```

```python
import functools

import jax
import jax.numpy as jnp
from jax import lax
from jax.experimental import pallas as pl
from jax.experimental.pallas import tpu as pltpu
from jax.sharding import PartitionSpec as P

norm_eps = 1e-05


def from_behind(value, axis, steps):
    count = lax.axis_size(axis)
    initial, last = (max(0, -steps), min(count, count - steps))
    return lax.ppermute(value, axis, [(source, source + steps) for source in range(initial, last)])


def stick_block(carry, query_heads, key_block, value_block, bias_block, query_pos, key_start):
    accum, kept_log = carry
    key_count = key_block.shape[0]
    head_count = query_heads.shape[1]
    key_heads = key_block.reshape(key_count, head_count, -1)
    value_heads = value_block.reshape(key_count, head_count, -1)
    scale = key_heads.shape[2] ** (-0.5)
    scores = (
        jnp.einsum("qhd,khd->hqk", query_heads, key_heads, preferred_element_type=jnp.float32)
        * scale
    )
    scores = scores + bias_block.astype(jnp.float32)[:, None, :]
    key_pos = key_start + lax.iota(jnp.int32, key_count)
    strict = ((key_pos[None, :] < query_pos[:, None]) & (key_pos[None, :] >= 0))[None]
    log_retained = jnp.where(strict, jax.nn.log_sigmoid(-scores), 0.0)
    between = lax.cumsum(log_retained, axis=2, reverse=True) - log_retained + kept_log[:, :, None]
    stick = jnp.where(strict, jnp.exp(jax.nn.log_sigmoid(scores) + between), 0.0).astype(
        jnp.bfloat16
    )
    accum = accum + jnp.einsum(
        "hqk,khd->qhd", stick, value_heads, preferred_element_type=jnp.float32
    )
    return (accum, kept_log + jnp.sum(log_retained, axis=2))


def normalize(middle_wide, norm_gain):
    mean_square = jnp.mean(middle_wide * middle_wide, axis=1, keepdims=True)
    return (middle_wide * lax.rsqrt(mean_square + norm_eps) * norm_gain.astype(jnp.float32)).astype(
        jnp.bfloat16
    )


def body(
    queries,
    key_rows,
    value_rows,
    key_bias,
    residual,
    out_weight,
    norm_gain,
    gate_weight,
    up_weight,
    down_weight,
):
    seg_rows = queries.shape[0]
    head_count = key_bias.shape[0]
    head_width = queries.shape[1] // head_count
    sp_count = lax.axis_size("sp")
    token_place = lax.axis_index("sp")
    query_heads = queries.reshape(seg_rows, head_count, head_width)
    query_pos = token_place * seg_rows + lax.iota(jnp.int32, seg_rows)
    start_carry = (
        jnp.zeros((seg_rows, head_count, head_width), jnp.float32),
        jnp.zeros((head_count, seg_rows), jnp.float32),
    )
    carry = stick_block(
        start_carry, query_heads, key_rows, value_rows, key_bias, query_pos, token_place * seg_rows
    )

    def advance(hop_index, state):
        carry_now, blocks = state
        blocks = from_behind((blocks[0], blocks[1], blocks[2]), "sp", 1)

        def attend(current):
            return stick_block(
                current,
                query_heads,
                blocks[0],
                blocks[1],
                blocks[2],
                query_pos,
                (token_place - hop_index) * seg_rows,
            )

        carry_now = lax.cond(token_place >= hop_index, attend, lambda current: current, carry_now)
        return (carry_now, blocks)

    carry, passed_blocks = lax.fori_loop(
        1, sp_count, advance, (carry, (key_rows, value_rows, key_bias))
    )
    attended = carry[0].reshape(seg_rows, head_count * head_width).astype(jnp.bfloat16)
    own_rows = seg_rows // lax.axis_size("tp")
    own_start = lax.axis_index("tp") * own_rows
    mixed = lax.psum_scatter(
        jnp.dot(attended, out_weight, preferred_element_type=jnp.float32).astype(jnp.bfloat16),
        "tp",
        scatter_dimension=0,
        tiled=True,
    ).astype(jnp.float32)
    own_residual = lax.dynamic_slice_in_dim(residual, own_start, own_rows, 0)
    middle = (own_residual.astype(jnp.float32) + mixed).astype(jnp.bfloat16)
    middle_wide = middle.astype(jnp.float32)
    normed_all = lax.all_gather(normalize(middle_wide, norm_gain), "tp", axis=0, tiled=True)
    gate_pre = jnp.dot(
        normed_all,
        lax.all_gather(gate_weight, "sp", axis=0, tiled=True),
        preferred_element_type=jnp.float32,
    )
    up_pre = jnp.dot(
        normed_all,
        lax.all_gather(up_weight, "sp", axis=0, tiled=True),
        preferred_element_type=jnp.float32,
    )
    hidden = (jax.nn.silu(gate_pre) * up_pre).astype(jnp.bfloat16)
    down_terms = jnp.dot(
        hidden,
        lax.all_gather(down_weight, "sp", axis=1, tiled=True),
        preferred_element_type=jnp.float32,
    )
    down_sum = lax.psum_scatter(
        down_terms.astype(jnp.bfloat16), "tp", scatter_dimension=0, tiled=True
    ).astype(jnp.float32)
    own_out = (middle_wide + down_sum).astype(jnp.bfloat16)
    return lax.all_gather(own_out, "tp", axis=0, tiled=True)


def contract(left, right, dims):
    return lax.dot_general(left, right, ((dims[:1], dims[1:]), ((), ())), preferred_element_type=jnp.float32)


def layer_kernel(
    grp_count,
    sp_count,
    tp_count,
    q_in,
    k_in,
    v_in,
    bias_in,
    res_in,
    ow_in,
    gain_in,
    gate_in,
    up_in,
    down_in,
    out_ref,
    q_ref,
    k_ref,
    v_ref,
    bias_ref,
    res_ref,
    ow_ref,
    gain_ref,
    gate_ref,
    up_ref,
    down_ref,
    load_sems,
    kbuf,
    vbuf,
    bbuf,
    acc,
    kept,
    wsend,
    w_all,
    pbuf,
    rbuf,
    middle,
    n_all,
    h_all,
    dbuf,
    rdown,
    zsend,
    zin,
    kv_sems,
    w_sems,
    wy_sems,
    r_sems,
    n_sems,
    f_sems,
    h_sems,
    d_sems,
    z_sems,
    o_sems,
):
    g, s, t = lax.axis_index("grp"), lax.axis_index("sp"), lax.axis_index("tp")
    rows, model = res_in.shape
    quarter = rows // tp_count
    slab = model // sp_count
    piece = gate_ref.shape[1] // sp_count
    head_count = bias_ref.shape[0]
    width = q_ref.shape[1] // head_count
    sends = []

    def sp_peer(step):
        return lax.rem(s + step + sp_count, sp_count)

    def tp_peer(step):
        return lax.rem(t + step + tp_count, tp_count)

    core_mate = t + 1 - 2 * lax.rem(t, 2)
    far_mate = lax.rem(t + 2, 4)

    def copy(source, target, sems, index, device):
        return pltpu.make_async_remote_copy(
            src_ref=source,
            dst_ref=target,
            send_sem=sems.at[(0,) + index],
            recv_sem=sems.at[(1,) + index],
            device_id=device,
            device_id_type=pl.DeviceIdType.MESH,
        )

    def launch(*arguments):
        made = copy(*arguments)
        made.start()
        sends.append(made)
        return made

    own_part = res_in.at[pl.ds(pl.multiple_of(t * quarter, quarter), quarter)]
    loads = {}
    for index, (name, source, target) in enumerate(
        (
            ("k", k_in, k_ref),
            ("v", v_in, v_ref),
            ("bias", bias_in, bias_ref),
            ("gate", gate_in, gate_ref),
            ("up", up_in, up_ref),
            ("q", q_in, q_ref),
            ("ow", ow_in, ow_ref),
            ("res", own_part, res_ref),
            ("gain", gain_in, gain_ref),
            ("down", down_in, down_ref),
        )
    ):
        loads[name] = pltpu.make_async_copy(source, target, load_sems.at[index])
        loads[name].start()

    barrier = pltpu.get_barrier_semaphore()
    for step in range(1, sp_count):
        pl.semaphore_signal(barrier, inc=1, device_id=(g, sp_peer(step), t), device_id_type=pl.DeviceIdType.MESH)
    for step in range(1, tp_count):
        pl.semaphore_signal(barrier, inc=1, device_id=(g, s, tp_peer(step)), device_id_type=pl.DeviceIdType.MESH)
    pl.semaphore_signal(barrier, inc=1, device_id=(1 - g, s, t), device_id_type=pl.DeviceIdType.MESH)
    pl.semaphore_wait(barrier, sp_count + tp_count - 1)

    for name in ("k", "v", "bias"):
        loads[name].wait()
    kv_copies = {}
    for step in range(1, sp_count):
        device = (g, sp_peer(step), t)
        kv_copies[step] = [
            copy(k_ref, kbuf.at[step - 1], kv_sems, (0, step - 1), device),
            copy(v_ref, vbuf.at[step - 1], kv_sems, (1, step - 1), device),
            copy(bias_ref, bbuf.at[step - 1], kv_sems, (2, step - 1), device),
        ]

        @pl.when(s + step < sp_count)
        def _():
            for made in kv_copies[step]:
                made.start()

    for name in ("gate", "up", "q"):
        loads[name].wait()
    for part, ref in ((0, gate_ref), (1, up_ref)):
        for start in range(0, ref.shape[1], 128):
            wsend[part, start : start + 128, :] = ref[:, start : start + 128].T
    w_copies = {}
    for step in range(1, sp_count):
        dest = sp_peer(step)
        w_copies[step] = launch(
            wsend.at[g, pl.ds(pl.multiple_of(dest * piece, 16), piece)],
            w_all.at[s, g],
            w_sems,
            (step - 1,),
            (g, dest, t),
        )
    for part in range(2):
        w_all[s, part] = wsend[part, pl.ds(pl.multiple_of(s * piece, 16), piece), :]

    acc[...] = jnp.zeros_like(acc)
    kept[...] = jnp.zeros_like(kept)
    query = q_ref[...]
    lane = lax.broadcasted_iota(jnp.int32, query.shape, 1)
    row_id = lax.broadcasted_iota(jnp.int32, (rows, rows), 0)
    col_id = lax.broadcasted_iota(jnp.int32, (rows, rows), 1)
    later = (row_id > col_id).astype(jnp.bfloat16)
    scale = width ** (-0.5)

    def attend(key_block, value_block, bias_block, diagonal):
        bias_wide = bias_block.astype(jnp.float32)
        for head in range(head_count):
            mine = (lane >= head * width) & (lane < (head + 1) * width)
            zero = jnp.zeros_like(query)
            scores = contract(jnp.where(mine, query, zero), key_block, (1, 1)) * scale
            scores = scores + bias_wide[head : head + 1, :]
            soft = jnp.log1p(jnp.exp(-jnp.abs(scores)))
            log_take = jnp.minimum(scores, 0.0) - soft
            log_keep = -jnp.maximum(scores, 0.0) - soft
            if diagonal:
                log_keep = jnp.where(col_id < row_id, log_keep, 0.0)
            high = log_keep.astype(jnp.bfloat16)
            low = (log_keep - high.astype(jnp.float32)).astype(jnp.bfloat16)
            between = contract(high, later, (1, 0)) + contract(low, later, (1, 0)) + kept[head]
            stick = jnp.exp(log_take + between)
            if diagonal:
                stick = jnp.where(col_id < row_id, stick, 0.0)
            acc[...] += contract(
                stick.astype(jnp.bfloat16), jnp.where(mine, value_block, zero), (1, 0)
            )
            kept[head] = kept[head] + jnp.sum(log_keep, axis=1, keepdims=True)

    attend(k_ref[...], v_ref[...], bias_ref[...], True)
    for step in range(1, sp_count):

        @pl.when(s >= step)
        def _():
            for made in kv_copies[step]:
                made.wait_recv()
            attend(kbuf[step - 1], vbuf[step - 1], bbuf[step - 1], False)

    for name in ("ow", "res", "gain", "down"):
        loads[name].wait()
    attended = acc[...].astype(jnp.bfloat16)
    for start in range(0, model, 512):
        pbuf[:, start : start + 512] = contract(
            attended, ow_ref[:, start : start + 512], (1, 0)
        ).astype(jnp.bfloat16)

    def own_rows(index):
        return pl.ds(pl.multiple_of(index * quarter, quarter), quarter)

    r_copies = []
    for step in range(1, tp_count):
        dest = tp_peer(step)
        r_copies.append(
            launch(pbuf.at[own_rows(dest)], rbuf.at[step - 1], r_sems, (step - 1,), (g, s, dest))
        )
    mixed = pbuf[own_rows(t), :].astype(jnp.float32)
    for index, made in enumerate(r_copies):
        made.wait_recv()
        mixed = mixed + rbuf[index].astype(jnp.float32)
    middle[...] = (res_ref[...].astype(jnp.float32) + mixed).astype(jnp.bfloat16)
    wide = middle[...].astype(jnp.float32)
    mean_square = jnp.mean(wide * wide, axis=1, keepdims=True)
    n_all[s, t] = (
        wide * lax.rsqrt(mean_square + norm_eps) * gain_ref[...].astype(jnp.float32).reshape(1, model)
    ).astype(jnp.bfloat16)

    n_copies = {}
    for step in range(1, sp_count):
        n_copies[step] = launch(
            n_all.at[s, t], n_all.at[s, t], n_sems, (step - 1,), (g, sp_peer(step), t)
        )

    def spread(ref, sems, index):
        return (
            launch(ref(t), ref(t), sems, (0, index), (g, s, far_mate)),
            launch(ref(t), ref(t), sems, (1, index), (g, s, core_mate)),
        )

    def finish(ref, sems, index, first):
        first[0].wait_recv()
        relayed = launch(ref(far_mate), ref(far_mate), sems, (2, index), (g, s, core_mate))
        first[1].wait_recv()
        relayed.wait_recv()

    def n_view(block):
        return lambda place: n_all.at[block, place]

    spreads = {0: spread(n_view(s), f_sems, 0)}
    y_copies = []
    for step in range(1, sp_count):
        w_copies[step].wait_recv()
        view = w_all.at[sp_peer(-step), g]
        y_copies.append(launch(view, view, wy_sems, (step - 1,), (1 - g, s, t)))

    def pass_on(step):
        if step < sp_count:
            n_copies[step].wait_recv()
            spreads[step] = spread(n_view(sp_peer(-step)), f_sems, step)

    pass_on(1)
    for made in y_copies:
        made.wait_recv()

    h_copies = {}
    for step in range(sp_count):
        block = sp_peer(-step)
        if step:
            pass_on(step + 1)
        finish(n_view(block), f_sems, step, spreads[step])
        total = jnp.zeros((2 * piece, rows), jnp.float32)
        tokens = n_all[block].reshape(rows, model)
        for part in range(sp_count):
            total = total + contract(
                w_all[part].reshape(2 * piece, slab),
                tokens[:, part * slab : (part + 1) * slab],
                (1, 1),
            )
        gate_pre, up_pre = total[:piece], total[piece:]
        h_all[block, s] = (gate_pre / (1.0 + jnp.exp(-gate_pre)) * up_pre).astype(jnp.bfloat16)
        for hop in range(1, sp_count):
            h_copies[step, hop] = launch(
                h_all.at[block, s], h_all.at[block, s], h_sems, (step, hop - 1), (g, sp_peer(hop), t)
            )

    d_copies = {}
    order = list(range(1, sp_count)) + [0]
    for step in order:
        block = sp_peer(-step)
        for hop in range(1, sp_count):
            h_copies[(step - hop) % sp_count, hop].wait_recv()
        hidden = h_all[block].reshape(sp_count * piece, rows)
        dbuf[block] = contract(hidden, down_ref[...], (0, 0)).astype(jnp.bfloat16)
        for hop in range(1, tp_count):
            dest = tp_peer(hop)
            d_copies[step, hop] = launch(
                dbuf.at[block, own_rows(dest)],
                rdown.at[hop - 1, step],
                d_sems,
                (step, hop - 1),
                (g, s, dest),
            )
    z_copies = {}
    for step in order:
        block = sp_peer(-step)
        summed = dbuf[block, own_rows(t), :].astype(jnp.float32)
        for hop in range(1, tp_count):
            d_copies[step, hop].wait_recv()
            summed = summed + rdown[hop - 1, step].astype(jnp.float32)
        if step:
            zsend[step - 1] = summed.astype(jnp.bfloat16)
            z_copies[step] = launch(
                zsend.at[step - 1], zin.at[s], z_sems, (step - 1,), (g, block, t)
            )
        else:
            zin[s] = summed.astype(jnp.bfloat16)
    for step in range(1, sp_count):
        z_copies[step].wait_recv()
    for part in range(sp_count):
        cols = slice(part * slab, (part + 1) * slab)
        out_ref[own_rows(t), cols] = (
            middle[:, cols].astype(jnp.float32) + zin[part].astype(jnp.float32)
        ).astype(jnp.bfloat16)

    def out_view(place):
        return out_ref.at[own_rows(place)]

    finish(out_view, o_sems, 0, spread(out_view, o_sems, 0))
    for made in sends:
        made.wait_send()
    for step in range(1, sp_count):

        @pl.when(s + step < sp_count)
        def _():
            for made in kv_copies[step]:
                made.wait_send()


def fused_body(
    grp_count,
    sp_count,
    tp_count,
    queries,
    key_rows,
    value_rows,
    key_bias,
    residual,
    out_weight,
    norm_gain,
    gate_weight,
    up_weight,
    down_weight,
):
    rows, columns = queries.shape
    head_count = key_bias.shape[0]
    model = residual.shape[1]
    hidden = gate_weight.shape[1]
    piece, slab, quarter = hidden // sp_count, model // sp_count, rows // tp_count
    n, m = sp_count - 1, tp_count - 1
    half, wide = jnp.bfloat16, jnp.float32
    dma = pltpu.SemaphoreType.DMA
    return pl.pallas_call(
        functools.partial(layer_kernel, grp_count, sp_count, tp_count),
        out_shape=jax.ShapeDtypeStruct((rows, model), half),
        in_specs=[pl.BlockSpec(memory_space=pl.ANY)] * 10,
        out_specs=pl.BlockSpec(memory_space=pltpu.VMEM),
        scratch_shapes=[
            pltpu.VMEM((rows, columns), half),
            pltpu.VMEM((rows, columns), half),
            pltpu.VMEM((rows, columns), half),
            pltpu.VMEM((head_count, rows), half),
            pltpu.VMEM((quarter, model), half),
            pltpu.VMEM((columns, model), half),
            pltpu.VMEM((model,), half),
            pltpu.VMEM((slab, hidden), half),
            pltpu.VMEM((slab, hidden), half),
            pltpu.VMEM((hidden, slab), half),
            dma((10,)),
            pltpu.VMEM((n, rows, columns), half),
            pltpu.VMEM((n, rows, columns), half),
            pltpu.VMEM((n, head_count, rows), half),
            pltpu.VMEM((rows, columns), wide),
            pltpu.VMEM((head_count, rows, 1), wide),
            pltpu.VMEM((2, hidden, slab), half),
            pltpu.VMEM((sp_count, 2, piece, slab), half),
            pltpu.VMEM((rows, model), half),
            pltpu.VMEM((m, quarter, model), half),
            pltpu.VMEM((quarter, model), half),
            pltpu.VMEM((sp_count, tp_count, quarter, model), half),
            pltpu.VMEM((sp_count, sp_count, piece, rows), half),
            pltpu.VMEM((sp_count, rows, slab), half),
            pltpu.VMEM((m, sp_count, quarter, slab), half),
            pltpu.VMEM((n, quarter, slab), half),
            pltpu.VMEM((sp_count, quarter, slab), half),
            dma((2, 3, n)),
            dma((2, n)),
            dma((2, n)),
            dma((2, m)),
            dma((2, n)),
            dma((2, 3, sp_count)),
            dma((2, sp_count, n)),
            dma((2, sp_count, m)),
            dma((2, n)),
            dma((2, 3, 1)),
        ],
        compiler_params=pltpu.CompilerParams(
            collective_id=0, has_side_effects=True, vmem_limit_bytes=67_043_328
        ),
    )(
        queries,
        key_rows,
        value_rows,
        key_bias,
        residual,
        out_weight,
        norm_gain,
        gate_weight,
        up_weight,
        down_weight,
    )


def any_body(sizes, *arguments):
    grp_count, sp_count, tp_count = sizes
    queries, model, hidden = arguments[0], arguments[4].shape[1], arguments[7].shape[1]
    rows = queries.shape[0]
    fits = (
        grp_count == 2
        and tp_count == 4
        and 1 < sp_count <= 4
        and rows == 128
        and queries.shape[1] == 128
        and (model // sp_count) % 128 == 0
        and (hidden // sp_count) % 16 == 0
        and hidden % 128 == 0
    )
    if fits:
        return fused_body(grp_count, sp_count, tp_count, *arguments)
    return body(*arguments)


def solution(mesh):
    in_specs = (
        P(("grp", "sp"), "tp"),
        P(("grp", "sp"), "tp"),
        P(("grp", "sp"), "tp"),
        P("tp", ("grp", "sp")),
        P(("grp", "sp"), None),
        P("tp", None),
        P(),
        P("sp", "tp"),
        P("sp", "tp"),
        P("tp", "sp"),
    )
    out_specs = P(("grp", "sp"), None)
    sizes = tuple(mesh.shape[name] for name in ("grp", "sp", "tp"))
    return jax.shard_map(functools.partial(any_body, sizes), mesh=mesh, in_specs=in_specs, out_specs=out_specs, check_vma=False)
```

```python
import functools

import jax
import jax.numpy as jnp
from jax import lax
from jax.experimental import pallas as pl
from jax.experimental.pallas import tpu as pltpu
from jax.sharding import PartitionSpec as P

norm_eps = 1e-05


def from_behind(value, axis, steps):
    count = lax.axis_size(axis)
    initial, last = (max(0, -steps), min(count, count - steps))
    return lax.ppermute(value, axis, [(source, source + steps) for source in range(initial, last)])


def stick_block(carry, query_heads, key_block, value_block, bias_block, query_pos, key_start):
    accum, kept_log = carry
    key_count = key_block.shape[0]
    head_count = query_heads.shape[1]
    key_heads = key_block.reshape(key_count, head_count, -1)
    value_heads = value_block.reshape(key_count, head_count, -1)
    scale = key_heads.shape[2] ** (-0.5)
    scores = (
        jnp.einsum("qhd,khd->hqk", query_heads, key_heads, preferred_element_type=jnp.float32)
        * scale
    )
    scores = scores + bias_block.astype(jnp.float32)[:, None, :]
    key_pos = key_start + lax.iota(jnp.int32, key_count)
    strict = ((key_pos[None, :] < query_pos[:, None]) & (key_pos[None, :] >= 0))[None]
    log_retained = jnp.where(strict, jax.nn.log_sigmoid(-scores), 0.0)
    between = lax.cumsum(log_retained, axis=2, reverse=True) - log_retained + kept_log[:, :, None]
    stick = jnp.where(strict, jnp.exp(jax.nn.log_sigmoid(scores) + between), 0.0).astype(
        jnp.bfloat16
    )
    accum = accum + jnp.einsum(
        "hqk,khd->qhd", stick, value_heads, preferred_element_type=jnp.float32
    )
    return (accum, kept_log + jnp.sum(log_retained, axis=2))


def normalize(middle_wide, norm_gain):
    mean_square = jnp.mean(middle_wide * middle_wide, axis=1, keepdims=True)
    return (middle_wide * lax.rsqrt(mean_square + norm_eps) * norm_gain.astype(jnp.float32)).astype(
        jnp.bfloat16
    )


def body(
    queries,
    key_rows,
    value_rows,
    key_bias,
    residual,
    out_weight,
    norm_gain,
    gate_weight,
    up_weight,
    down_weight,
):
    seg_rows = queries.shape[0]
    head_count = key_bias.shape[0]
    head_width = queries.shape[1] // head_count
    sp_count = lax.axis_size("sp")
    token_place = lax.axis_index("sp")
    query_heads = queries.reshape(seg_rows, head_count, head_width)
    query_pos = token_place * seg_rows + lax.iota(jnp.int32, seg_rows)
    start_carry = (
        jnp.zeros((seg_rows, head_count, head_width), jnp.float32),
        jnp.zeros((head_count, seg_rows), jnp.float32),
    )
    carry = stick_block(
        start_carry, query_heads, key_rows, value_rows, key_bias, query_pos, token_place * seg_rows
    )

    def advance(hop_index, state):
        carry_now, blocks = state
        blocks = from_behind((blocks[0], blocks[1], blocks[2]), "sp", 1)

        def attend(current):
            return stick_block(
                current,
                query_heads,
                blocks[0],
                blocks[1],
                blocks[2],
                query_pos,
                (token_place - hop_index) * seg_rows,
            )

        carry_now = lax.cond(token_place >= hop_index, attend, lambda current: current, carry_now)
        return (carry_now, blocks)

    carry, passed_blocks = lax.fori_loop(
        1, sp_count, advance, (carry, (key_rows, value_rows, key_bias))
    )
    attended = carry[0].reshape(seg_rows, head_count * head_width).astype(jnp.bfloat16)
    own_rows = seg_rows // lax.axis_size("tp")
    own_start = lax.axis_index("tp") * own_rows
    mixed = lax.psum_scatter(
        jnp.dot(attended, out_weight, preferred_element_type=jnp.float32).astype(jnp.bfloat16),
        "tp",
        scatter_dimension=0,
        tiled=True,
    ).astype(jnp.float32)
    own_residual = lax.dynamic_slice_in_dim(residual, own_start, own_rows, 0)
    middle = (own_residual.astype(jnp.float32) + mixed).astype(jnp.bfloat16)
    middle_wide = middle.astype(jnp.float32)
    normed_all = lax.all_gather(normalize(middle_wide, norm_gain), "tp", axis=0, tiled=True)
    gate_pre = jnp.dot(
        normed_all,
        lax.all_gather(gate_weight, "sp", axis=0, tiled=True),
        preferred_element_type=jnp.float32,
    )
    up_pre = jnp.dot(
        normed_all,
        lax.all_gather(up_weight, "sp", axis=0, tiled=True),
        preferred_element_type=jnp.float32,
    )
    hidden = (jax.nn.silu(gate_pre) * up_pre).astype(jnp.bfloat16)
    down_terms = jnp.dot(
        hidden,
        lax.all_gather(down_weight, "sp", axis=1, tiled=True),
        preferred_element_type=jnp.float32,
    )
    down_sum = lax.psum_scatter(
        down_terms.astype(jnp.bfloat16), "tp", scatter_dimension=0, tiled=True
    ).astype(jnp.float32)
    own_out = (middle_wide + down_sum).astype(jnp.bfloat16)
    return lax.all_gather(own_out, "tp", axis=0, tiled=True)


def contract(left, right, dims):
    return lax.dot_general(left, right, ((dims[:1], dims[1:]), ((), ())), preferred_element_type=jnp.float32)


def layer_kernel(
    grp_count,
    sp_count,
    tp_count,
    q_in,
    k_in,
    v_in,
    bias_in,
    res_in,
    ow_in,
    gain_in,
    gate_in,
    up_in,
    down_in,
    out_ref,
    q_ref,
    k_ref,
    v_ref,
    bias_ref,
    res_ref,
    ow_ref,
    gain_ref,
    gate_ref,
    up_ref,
    down_ref,
    load_sems,
    kbuf,
    vbuf,
    bbuf,
    acc,
    kept,
    wsend,
    w_all,
    pbuf,
    rbuf,
    middle,
    n_all,
    h_all,
    dbuf,
    rdown,
    zsend,
    zin,
    kv_sems,
    w_sems,
    wy_sems,
    r_sems,
    n_sems,
    f_sems,
    h_sems,
    d_sems,
    z_sems,
    o_sems,
):
    g, s, t = lax.axis_index("grp"), lax.axis_index("sp"), lax.axis_index("tp")
    rows, model = res_in.shape
    quarter = rows // tp_count
    slab = model // sp_count
    piece = gate_ref.shape[1] // sp_count
    head_count = bias_ref.shape[0]
    width = q_ref.shape[1] // head_count
    sends, guarded = [], []

    def sp_peer(step):
        return lax.rem(s + step + sp_count, sp_count)

    def tp_peer(step):
        return lax.rem(t + step + tp_count, tp_count)

    core_mate = t + 1 - 2 * lax.rem(t, 2)
    far_mate = lax.rem(t + 2, 4)

    def copy(source, target, sems, index, device):
        return pltpu.make_async_remote_copy(
            src_ref=source,
            dst_ref=target,
            send_sem=sems.at[(0,) + index],
            recv_sem=sems.at[(1,) + index],
            device_id=device,
            device_id_type=pl.DeviceIdType.MESH,
        )

    def launch(*arguments):
        made = copy(*arguments)
        made.start()
        sends.append(made)
        return made

    own_part = res_in.at[pl.ds(pl.multiple_of(t * quarter, quarter), quarter)]
    loads = {}
    for index, (name, source, target) in enumerate(
        (
            ("k", k_in, k_ref),
            ("v", v_in, v_ref),
            ("bias", bias_in, bias_ref),
            ("gate", gate_in, gate_ref),
            ("up", up_in, up_ref),
            ("q", q_in, q_ref),
            ("ow", ow_in, ow_ref),
            ("res", own_part, res_ref),
            ("gain", gain_in, gain_ref),
            ("down", down_in, down_ref),
        )
    ):
        loads[name] = pltpu.make_async_copy(source, target, load_sems.at[index])
        loads[name].start()

    barrier = pltpu.get_barrier_semaphore()
    for step in range(1, sp_count):
        pl.semaphore_signal(barrier, inc=1, device_id=(g, sp_peer(step), t), device_id_type=pl.DeviceIdType.MESH)
    for step in range(1, tp_count):
        pl.semaphore_signal(barrier, inc=1, device_id=(g, s, tp_peer(step)), device_id_type=pl.DeviceIdType.MESH)
    pl.semaphore_signal(barrier, inc=1, device_id=(1 - g, s, t), device_id_type=pl.DeviceIdType.MESH)
    pl.semaphore_wait(barrier, sp_count + tp_count - 1)

    for name in ("k", "v", "bias"):
        loads[name].wait()
    kv_copies = {}
    for step in range(1, sp_count):
        device = (g, sp_peer(step), t)
        kv_copies[step] = [
            copy(k_ref, kbuf.at[step - 1], kv_sems, (0, step - 1), device),
            copy(v_ref, vbuf.at[step - 1], kv_sems, (1, step - 1), device),
            copy(bias_ref, bbuf.at[step - 1], kv_sems, (2, step - 1), device),
        ]

        @pl.when(s + step < sp_count)
        def _():
            for made in kv_copies[step]:
                made.start()

    for name in ("gate", "up", "q"):
        loads[name].wait()
    for part, ref in ((0, gate_ref), (1, up_ref)):
        for start in range(0, ref.shape[1], 128):
            wsend[part, start : start + 128, :] = ref[:, start : start + 128].T
    w_copies = {}
    for step in range(1, sp_count):
        dest = sp_peer(step)
        w_copies[step] = launch(
            wsend.at[g, pl.ds(pl.multiple_of(dest * piece, 16), piece)],
            w_all.at[s, g],
            w_sems,
            (step - 1,),
            (g, dest, t),
        )
    for part in range(2):
        w_all[s, part] = wsend[part, pl.ds(pl.multiple_of(s * piece, 16), piece), :]

    acc[...] = jnp.zeros_like(acc)
    kept[...] = jnp.zeros_like(kept)
    query = q_ref[...]
    lane = lax.broadcasted_iota(jnp.int32, query.shape, 1)
    row_id = lax.broadcasted_iota(jnp.int32, (rows, rows), 0)
    col_id = lax.broadcasted_iota(jnp.int32, (rows, rows), 1)
    later = (row_id > col_id).astype(jnp.bfloat16)
    scale = width ** (-0.5)

    def attend(key_block, value_block, bias_block, diagonal):
        bias_wide = bias_block.astype(jnp.float32)
        for head in range(head_count):
            mine = (lane >= head * width) & (lane < (head + 1) * width)
            zero = jnp.zeros_like(query)
            scores = contract(jnp.where(mine, query, zero), key_block, (1, 1)) * scale
            scores = scores + bias_wide[head : head + 1, :]
            soft = jnp.log1p(jnp.exp(-jnp.abs(scores)))
            log_take = jnp.minimum(scores, 0.0) - soft
            log_keep = -jnp.maximum(scores, 0.0) - soft
            if diagonal:
                log_keep = jnp.where(col_id < row_id, log_keep, 0.0)
            high = log_keep.astype(jnp.bfloat16)
            low = (log_keep - high.astype(jnp.float32)).astype(jnp.bfloat16)
            between = contract(high, later, (1, 0)) + contract(low, later, (1, 0)) + kept[head]
            stick = jnp.exp(log_take + between)
            if diagonal:
                stick = jnp.where(col_id < row_id, stick, 0.0)
            acc[...] += contract(
                stick.astype(jnp.bfloat16), jnp.where(mine, value_block, zero), (1, 0)
            )
            kept[head] = kept[head] + jnp.sum(log_keep, axis=1, keepdims=True)

    attend(k_ref[...], v_ref[...], bias_ref[...], True)
    for step in range(1, sp_count):

        @pl.when(s >= step)
        def _():
            for made in kv_copies[step]:
                made.wait_recv()
            attend(kbuf[step - 1], vbuf[step - 1], bbuf[step - 1], False)

    for name in ("ow", "res", "gain", "down"):
        loads[name].wait()
    attended = acc[...].astype(jnp.bfloat16)
    for start in range(0, model, 512):
        pbuf[:, start : start + 512] = contract(
            attended, ow_ref[:, start : start + 512], (1, 0)
        ).astype(jnp.bfloat16)

    def own_rows(index):
        return pl.ds(pl.multiple_of(index * quarter, quarter), quarter)

    r_copies = []
    for step in range(1, tp_count):
        dest = tp_peer(step)
        r_copies.append(
            launch(pbuf.at[own_rows(dest)], rbuf.at[step - 1], r_sems, (step - 1,), (g, s, dest))
        )
    mixed = pbuf[own_rows(t), :].astype(jnp.float32)
    for index, made in enumerate(r_copies):
        made.wait_recv()
        mixed = mixed + rbuf[index].astype(jnp.float32)
    middle[...] = (res_ref[...].astype(jnp.float32) + mixed).astype(jnp.bfloat16)
    wide = middle[...].astype(jnp.float32)
    mean_square = jnp.mean(wide * wide, axis=1, keepdims=True)
    n_all[s, t] = (
        wide * lax.rsqrt(mean_square + norm_eps) * gain_ref[...].astype(jnp.float32).reshape(1, model)
    ).astype(jnp.bfloat16)

    up, down = 0, 1
    slots = [(step, way) for step in range(1, sp_count) for way in (up, down)]

    def place_of(origin, step, way):
        return origin - step if way == up else origin + step

    def inside(place):
        return (place >= 0) & (place < sp_count)

    def wrap(place):
        return lax.rem(place + 2 * sp_count, sp_count)

    def chain_copy(view, sems, way, hop, index):
        onward = wrap(s + 1 if way == up else s - 1)
        return copy(view, view, sems, (way, hop) + index, (g, onward, t))

    def chain_start(view, sems, way, hop, index, valid):
        going = valid & inside(s + 1 if way == up else s - 1)
        made = chain_copy(view, sems, way, hop, index)
        pl.when(going)(made.start)
        guarded.append((going, made))

    def spread(ref, sems, index, valid):
        first = (
            copy(ref(t), ref(t), sems, (0, index), (g, s, far_mate)),
            copy(ref(t), ref(t), sems, (1, index), (g, s, core_mate)),
        )
        for made in first:
            pl.when(valid)(made.start)
            guarded.append((valid, made))
        return first

    def finish(ref, sems, index, first, valid):
        relayed = copy(ref(far_mate), ref(far_mate), sems, (2, index), (g, s, core_mate))

        @pl.when(valid)
        def _():
            first[0].wait_recv()
            relayed.start()
            first[1].wait_recv()
            relayed.wait_recv()

        guarded.append((valid, relayed))

    def n_view(block):
        return lambda place: n_all.at[block, place]

    def slot_number(slot):
        return 0 if slot is None else 1 + slots.index(slot)

    always = s >= 0
    spreads = {}

    def arrive(slot):
        step, way = slot
        origin = place_of(s, step, way)
        valid, block = inside(origin), wrap(origin)
        view = n_all.at[block, t]
        pl.when(valid)(chain_copy(view, n_sems, way, step - 1, ()).wait_recv)
        if step < sp_count - 1:
            chain_start(view, n_sems, way, step, (), valid)
        spreads[slot] = spread(n_view(block), f_sems, slot_number(slot), valid)

    def process(slot):
        origin = s if slot is None else place_of(s, *slot)
        valid = always if slot is None else inside(origin)
        block = wrap(origin)
        number = slot_number(slot)
        finish(n_view(block), f_sems, number, spreads[slot], valid)

        @pl.when(valid)
        def _():
            total = jnp.zeros((2 * piece, rows), jnp.float32)
            tokens = n_all[block].reshape(rows, model)
            for part in range(sp_count):
                total = total + contract(
                    w_all[part].reshape(2 * piece, slab),
                    tokens[:, part * slab : (part + 1) * slab],
                    (1, 1),
                )
            gate_pre, up_pre = total[:piece], total[piece:]
            h_all[block, s] = (gate_pre / (1.0 + jnp.exp(-gate_pre)) * up_pre).astype(jnp.bfloat16)

        for way in (up, down):
            chain_start(h_all.at[block, s], h_sems, way, 0, (number,), valid)

    def hop_on(slot, step, way):
        if slot is not None and slot[1] == way and slot[0] + step >= sp_count:
            return
        source = place_of(s, step, way)
        target = source if slot is None else place_of(source, *slot)
        valid = inside(source) & inside(target)
        view, index = h_all.at[wrap(target), wrap(source)], (slot_number(slot),)
        pl.when(valid)(chain_copy(view, h_sems, way, step - 1, index).wait_recv)
        if step < sp_count - 1:
            chain_start(view, h_sems, way, step, index, valid)

    def hop_all(stage):
        for distance in range(stage):
            step = stage - distance
            if step < sp_count and distance < sp_count:
                for slot in [None] if distance == 0 else [(distance, up), (distance, down)]:
                    for way in (up, down):
                        hop_on(slot, step, way)

    for way in (up, down):
        chain_start(n_all.at[s, t], n_sems, way, 0, (), always)
    spreads[None] = spread(n_view(s), f_sems, 0, always)
    y_copies = []
    for step in range(1, sp_count):
        w_copies[step].wait_recv()
        view = w_all.at[sp_peer(-step), g]
        y_copies.append(launch(view, view, wy_sems, (step - 1,), (1 - g, s, t)))
    arrive((1, up))
    arrive((1, down))
    for made in y_copies:
        made.wait_recv()
    process(None)
    for stage in range(1, sp_count):
        for way in (up, down):
            if stage < sp_count - 1:
                arrive((stage + 1, way))
        for way in (up, down):
            process((stage, way))
        hop_all(stage)
    for stage in range(sp_count, 2 * sp_count - 1):
        hop_all(stage)

    d_copies = {}
    order = list(range(1, sp_count)) + [0]
    for step in order:
        block = sp_peer(-step)
        hidden = h_all[block].reshape(sp_count * piece, rows)
        dbuf[block] = contract(hidden, down_ref[...], (0, 0)).astype(jnp.bfloat16)
        for hop in range(1, tp_count):
            dest = tp_peer(hop)
            d_copies[step, hop] = launch(
                dbuf.at[block, own_rows(dest)],
                rdown.at[hop - 1, step],
                d_sems,
                (step, hop - 1),
                (g, s, dest),
            )
    z_copies = {}
    for step in order:
        block = sp_peer(-step)
        summed = dbuf[block, own_rows(t), :].astype(jnp.float32)
        for hop in range(1, tp_count):
            d_copies[step, hop].wait_recv()
            summed = summed + rdown[hop - 1, step].astype(jnp.float32)
        if step:
            zsend[step - 1] = summed.astype(jnp.bfloat16)
            z_copies[step] = launch(
                zsend.at[step - 1], zin.at[s], z_sems, (step - 1,), (g, block, t)
            )
        else:
            zin[s] = summed.astype(jnp.bfloat16)
    for step in range(1, sp_count):
        z_copies[step].wait_recv()
    for part in range(sp_count):
        cols = slice(part * slab, (part + 1) * slab)
        out_ref[own_rows(t), cols] = (
            middle[:, cols].astype(jnp.float32) + zin[part].astype(jnp.float32)
        ).astype(jnp.bfloat16)

    def out_view(place):
        return out_ref.at[own_rows(place)]

    finish(out_view, o_sems, 0, spread(out_view, o_sems, 0, always), always)
    for made in sends:
        made.wait_send()
    for valid, made in guarded:
        pl.when(valid)(made.wait_send)
    for step in range(1, sp_count):

        @pl.when(s + step < sp_count)
        def _():
            for made in kv_copies[step]:
                made.wait_send()


def fused_body(
    grp_count,
    sp_count,
    tp_count,
    queries,
    key_rows,
    value_rows,
    key_bias,
    residual,
    out_weight,
    norm_gain,
    gate_weight,
    up_weight,
    down_weight,
):
    rows, columns = queries.shape
    head_count = key_bias.shape[0]
    model = residual.shape[1]
    hidden = gate_weight.shape[1]
    piece, slab, quarter = hidden // sp_count, model // sp_count, rows // tp_count
    n, m = sp_count - 1, tp_count - 1
    half, wide = jnp.bfloat16, jnp.float32
    dma = pltpu.SemaphoreType.DMA
    return pl.pallas_call(
        functools.partial(layer_kernel, grp_count, sp_count, tp_count),
        out_shape=jax.ShapeDtypeStruct((rows, model), half),
        in_specs=[pl.BlockSpec(memory_space=pl.ANY)] * 10,
        out_specs=pl.BlockSpec(memory_space=pltpu.VMEM),
        scratch_shapes=[
            pltpu.VMEM((rows, columns), half),
            pltpu.VMEM((rows, columns), half),
            pltpu.VMEM((rows, columns), half),
            pltpu.VMEM((head_count, rows), half),
            pltpu.VMEM((quarter, model), half),
            pltpu.VMEM((columns, model), half),
            pltpu.VMEM((model,), half),
            pltpu.VMEM((slab, hidden), half),
            pltpu.VMEM((slab, hidden), half),
            pltpu.VMEM((hidden, slab), half),
            dma((10,)),
            pltpu.VMEM((n, rows, columns), half),
            pltpu.VMEM((n, rows, columns), half),
            pltpu.VMEM((n, head_count, rows), half),
            pltpu.VMEM((rows, columns), wide),
            pltpu.VMEM((head_count, rows, 1), wide),
            pltpu.VMEM((2, hidden, slab), half),
            pltpu.VMEM((sp_count, 2, piece, slab), half),
            pltpu.VMEM((rows, model), half),
            pltpu.VMEM((m, quarter, model), half),
            pltpu.VMEM((quarter, model), half),
            pltpu.VMEM((sp_count, tp_count, quarter, model), half),
            pltpu.VMEM((sp_count, sp_count, piece, rows), half),
            pltpu.VMEM((sp_count, rows, slab), half),
            pltpu.VMEM((m, sp_count, quarter, slab), half),
            pltpu.VMEM((n, quarter, slab), half),
            pltpu.VMEM((sp_count, quarter, slab), half),
            dma((2, 3, n)),
            dma((2, n)),
            dma((2, n)),
            dma((2, m)),
            dma((2, 2, n)),
            dma((2, 3, 2 * n + 1)),
            dma((2, 2, n, 2 * n + 1)),
            dma((2, sp_count, m)),
            dma((2, n)),
            dma((2, 3, 1)),
        ],
        compiler_params=pltpu.CompilerParams(
            collective_id=0, has_side_effects=True, vmem_limit_bytes=67_043_328
        ),
    )(
        queries,
        key_rows,
        value_rows,
        key_bias,
        residual,
        out_weight,
        norm_gain,
        gate_weight,
        up_weight,
        down_weight,
    )


def any_body(sizes, *arguments):
    grp_count, sp_count, tp_count = sizes
    queries, model, hidden = arguments[0], arguments[4].shape[1], arguments[7].shape[1]
    rows = queries.shape[0]
    fits = (
        grp_count == 2
        and tp_count == 4
        and 1 < sp_count <= 4
        and rows == 128
        and queries.shape[1] == 128
        and (model // sp_count) % 128 == 0
        and (hidden // sp_count) % 16 == 0
        and hidden % 128 == 0
    )
    if fits:
        return fused_body(grp_count, sp_count, tp_count, *arguments)
    return body(*arguments)


def solution(mesh):
    in_specs = (
        P(("grp", "sp"), "tp"),
        P(("grp", "sp"), "tp"),
        P(("grp", "sp"), "tp"),
        P("tp", ("grp", "sp")),
        P(("grp", "sp"), None),
        P("tp", None),
        P(),
        P("sp", "tp"),
        P("sp", "tp"),
        P("tp", "sp"),
    )
    out_specs = P(("grp", "sp"), None)
    sizes = tuple(mesh.shape[name] for name in ("grp", "sp", "tp"))
    return jax.shard_map(functools.partial(any_body, sizes), mesh=mesh, in_specs=in_specs, out_specs=out_specs, check_vma=False)
```

```python
import functools

import jax
import jax.numpy as jnp
from jax import lax
from jax.experimental import pallas as pl
from jax.experimental.pallas import tpu as pltpu
from jax.sharding import PartitionSpec as P

norm_eps = 1e-05


def from_behind(value, axis, steps):
    count = lax.axis_size(axis)
    initial, last = (max(0, -steps), min(count, count - steps))
    return lax.ppermute(value, axis, [(source, source + steps) for source in range(initial, last)])


def stick_block(carry, query_heads, key_block, value_block, bias_block, query_pos, key_start):
    accum, kept_log = carry
    key_count = key_block.shape[0]
    head_count = query_heads.shape[1]
    key_heads = key_block.reshape(key_count, head_count, -1)
    value_heads = value_block.reshape(key_count, head_count, -1)
    scale = key_heads.shape[2] ** (-0.5)
    scores = (
        jnp.einsum("qhd,khd->hqk", query_heads, key_heads, preferred_element_type=jnp.float32)
        * scale
    )
    scores = scores + bias_block.astype(jnp.float32)[:, None, :]
    key_pos = key_start + lax.iota(jnp.int32, key_count)
    strict = ((key_pos[None, :] < query_pos[:, None]) & (key_pos[None, :] >= 0))[None]
    log_retained = jnp.where(strict, jax.nn.log_sigmoid(-scores), 0.0)
    between = lax.cumsum(log_retained, axis=2, reverse=True) - log_retained + kept_log[:, :, None]
    stick = jnp.where(strict, jnp.exp(jax.nn.log_sigmoid(scores) + between), 0.0).astype(
        jnp.bfloat16
    )
    accum = accum + jnp.einsum(
        "hqk,khd->qhd", stick, value_heads, preferred_element_type=jnp.float32
    )
    return (accum, kept_log + jnp.sum(log_retained, axis=2))


def normalize(middle_wide, norm_gain):
    mean_square = jnp.mean(middle_wide * middle_wide, axis=1, keepdims=True)
    return (middle_wide * lax.rsqrt(mean_square + norm_eps) * norm_gain.astype(jnp.float32)).astype(
        jnp.bfloat16
    )


def body(
    queries,
    key_rows,
    value_rows,
    key_bias,
    residual,
    out_weight,
    norm_gain,
    gate_weight,
    up_weight,
    down_weight,
):
    seg_rows = queries.shape[0]
    head_count = key_bias.shape[0]
    head_width = queries.shape[1] // head_count
    sp_count = lax.axis_size("sp")
    token_place = lax.axis_index("sp")
    query_heads = queries.reshape(seg_rows, head_count, head_width)
    query_pos = token_place * seg_rows + lax.iota(jnp.int32, seg_rows)
    start_carry = (
        jnp.zeros((seg_rows, head_count, head_width), jnp.float32),
        jnp.zeros((head_count, seg_rows), jnp.float32),
    )
    carry = stick_block(
        start_carry, query_heads, key_rows, value_rows, key_bias, query_pos, token_place * seg_rows
    )

    def advance(hop_index, state):
        carry_now, blocks = state
        blocks = from_behind((blocks[0], blocks[1], blocks[2]), "sp", 1)

        def attend(current):
            return stick_block(
                current,
                query_heads,
                blocks[0],
                blocks[1],
                blocks[2],
                query_pos,
                (token_place - hop_index) * seg_rows,
            )

        carry_now = lax.cond(token_place >= hop_index, attend, lambda current: current, carry_now)
        return (carry_now, blocks)

    carry, passed_blocks = lax.fori_loop(
        1, sp_count, advance, (carry, (key_rows, value_rows, key_bias))
    )
    attended = carry[0].reshape(seg_rows, head_count * head_width).astype(jnp.bfloat16)
    own_rows = seg_rows // lax.axis_size("tp")
    own_start = lax.axis_index("tp") * own_rows
    mixed = lax.psum_scatter(
        jnp.dot(attended, out_weight, preferred_element_type=jnp.float32).astype(jnp.bfloat16),
        "tp",
        scatter_dimension=0,
        tiled=True,
    ).astype(jnp.float32)
    own_residual = lax.dynamic_slice_in_dim(residual, own_start, own_rows, 0)
    middle = (own_residual.astype(jnp.float32) + mixed).astype(jnp.bfloat16)
    middle_wide = middle.astype(jnp.float32)
    normed_all = lax.all_gather(normalize(middle_wide, norm_gain), "tp", axis=0, tiled=True)
    gate_pre = jnp.dot(
        normed_all,
        lax.all_gather(gate_weight, "sp", axis=0, tiled=True),
        preferred_element_type=jnp.float32,
    )
    up_pre = jnp.dot(
        normed_all,
        lax.all_gather(up_weight, "sp", axis=0, tiled=True),
        preferred_element_type=jnp.float32,
    )
    hidden = (jax.nn.silu(gate_pre) * up_pre).astype(jnp.bfloat16)
    down_terms = jnp.dot(
        hidden,
        lax.all_gather(down_weight, "sp", axis=1, tiled=True),
        preferred_element_type=jnp.float32,
    )
    down_sum = lax.psum_scatter(
        down_terms.astype(jnp.bfloat16), "tp", scatter_dimension=0, tiled=True
    ).astype(jnp.float32)
    own_out = (middle_wide + down_sum).astype(jnp.bfloat16)
    return lax.all_gather(own_out, "tp", axis=0, tiled=True)


def contract(left, right, dims):
    return lax.dot_general(left, right, ((dims[:1], dims[1:]), ((), ())), preferred_element_type=jnp.float32)


def layer_kernel(
    grp_count,
    sp_count,
    tp_count,
    q_in,
    k_in,
    v_in,
    bias_in,
    res_in,
    ow_in,
    gain_in,
    gate_in,
    up_in,
    down_in,
    out_ref,
    q_ref,
    k_ref,
    v_ref,
    bias_ref,
    res_ref,
    ow_ref,
    gain_ref,
    gate_ref,
    up_ref,
    down_ref,
    load_sems,
    kbuf,
    vbuf,
    bbuf,
    acc,
    kept,
    wsend,
    w_all,
    pbuf,
    rbuf,
    middle,
    n_all,
    h_all,
    dbuf,
    rdown,
    psend,
    zsend,
    zin,
    kv_sems,
    w_sems,
    wy_sems,
    r_sems,
    n_sems,
    f_sems,
    h_sems,
    d_sems,
    z_sems,
    o_sems,
):
    g, s, t = lax.axis_index("grp"), lax.axis_index("sp"), lax.axis_index("tp")
    rows, model = res_in.shape
    quarter = rows // tp_count
    slab = model // sp_count
    piece = gate_ref.shape[1] // sp_count
    head_count = bias_ref.shape[0]
    width = q_ref.shape[1] // head_count
    sends, guarded = [], []

    def sp_peer(step):
        return lax.rem(s + step + sp_count, sp_count)

    def tp_peer(step):
        return lax.rem(t + step + tp_count, tp_count)

    core_mate = t + 1 - 2 * lax.rem(t, 2)
    far_mate = lax.rem(t + 2, 4)

    def copy(source, target, sems, index, device):
        return pltpu.make_async_remote_copy(
            src_ref=source,
            dst_ref=target,
            send_sem=sems.at[(0,) + index],
            recv_sem=sems.at[(1,) + index],
            device_id=device,
            device_id_type=pl.DeviceIdType.MESH,
        )

    def launch(*arguments):
        made = copy(*arguments)
        made.start()
        sends.append(made)
        return made

    own_part = res_in.at[pl.ds(pl.multiple_of(t * quarter, quarter), quarter)]
    loads = {}
    for index, (name, source, target) in enumerate(
        (
            ("k", k_in, k_ref),
            ("v", v_in, v_ref),
            ("bias", bias_in, bias_ref),
            ("gate", gate_in, gate_ref),
            ("up", up_in, up_ref),
            ("q", q_in, q_ref),
            ("ow", ow_in, ow_ref),
            ("res", own_part, res_ref),
            ("gain", gain_in, gain_ref),
            ("down", down_in, down_ref),
        )
    ):
        loads[name] = pltpu.make_async_copy(source, target, load_sems.at[index])
        loads[name].start()

    barrier = pltpu.get_barrier_semaphore()
    for step in range(1, sp_count):
        pl.semaphore_signal(barrier, inc=1, device_id=(g, sp_peer(step), t), device_id_type=pl.DeviceIdType.MESH)
    for step in range(1, tp_count):
        pl.semaphore_signal(barrier, inc=1, device_id=(g, s, tp_peer(step)), device_id_type=pl.DeviceIdType.MESH)
    pl.semaphore_signal(barrier, inc=1, device_id=(1 - g, s, t), device_id_type=pl.DeviceIdType.MESH)
    pl.semaphore_wait(barrier, sp_count + tp_count - 1)

    for name in ("k", "v", "bias"):
        loads[name].wait()
    kv_copies = {}
    for step in range(1, sp_count):
        device = (g, sp_peer(step), t)
        kv_copies[step] = [
            copy(k_ref, kbuf.at[step - 1], kv_sems, (0, step - 1), device),
            copy(v_ref, vbuf.at[step - 1], kv_sems, (1, step - 1), device),
            copy(bias_ref, bbuf.at[step - 1], kv_sems, (2, step - 1), device),
        ]

        @pl.when(s + step < sp_count)
        def _():
            for made in kv_copies[step]:
                made.start()

    for name in ("gate", "up", "q"):
        loads[name].wait()
    for part, ref in ((0, gate_ref), (1, up_ref)):
        for start in range(0, ref.shape[1], 128):
            wsend[part, start : start + 128, :] = ref[:, start : start + 128].T
    w_copies = {}
    for step in range(1, sp_count):
        dest = sp_peer(step)
        w_copies[step] = launch(
            wsend.at[g, pl.ds(pl.multiple_of(dest * piece, 16), piece)],
            w_all.at[s, g],
            w_sems,
            (step - 1,),
            (g, dest, t),
        )
    for part in range(2):
        w_all[s, part] = wsend[part, pl.ds(pl.multiple_of(s * piece, 16), piece), :]

    acc[...] = jnp.zeros_like(acc)
    kept[...] = jnp.zeros_like(kept)
    query = q_ref[...]
    lane = lax.broadcasted_iota(jnp.int32, query.shape, 1)
    row_id = lax.broadcasted_iota(jnp.int32, (rows, rows), 0)
    col_id = lax.broadcasted_iota(jnp.int32, (rows, rows), 1)
    later = (row_id > col_id).astype(jnp.bfloat16)
    scale = width ** (-0.5)

    def attend(key_block, value_block, bias_block, diagonal):
        bias_wide = bias_block.astype(jnp.float32)
        for head in range(head_count):
            mine = (lane >= head * width) & (lane < (head + 1) * width)
            zero = jnp.zeros_like(query)
            scores = contract(jnp.where(mine, query, zero), key_block, (1, 1)) * scale
            scores = scores + bias_wide[head : head + 1, :]
            soft = jnp.log1p(jnp.exp(-jnp.abs(scores)))
            log_take = jnp.minimum(scores, 0.0) - soft
            log_keep = -jnp.maximum(scores, 0.0) - soft
            if diagonal:
                log_keep = jnp.where(col_id < row_id, log_keep, 0.0)
            high = log_keep.astype(jnp.bfloat16)
            low = (log_keep - high.astype(jnp.float32)).astype(jnp.bfloat16)
            between = contract(high, later, (1, 0)) + contract(low, later, (1, 0)) + kept[head]
            stick = jnp.exp(log_take + between)
            if diagonal:
                stick = jnp.where(col_id < row_id, stick, 0.0)
            acc[...] += contract(
                stick.astype(jnp.bfloat16), jnp.where(mine, value_block, zero), (1, 0)
            )
            kept[head] = kept[head] + jnp.sum(log_keep, axis=1, keepdims=True)

    attend(k_ref[...], v_ref[...], bias_ref[...], True)
    for step in range(1, sp_count):

        @pl.when(s >= step)
        def _():
            for made in kv_copies[step]:
                made.wait_recv()
            attend(kbuf[step - 1], vbuf[step - 1], bbuf[step - 1], False)

    for name in ("ow", "res", "gain", "down"):
        loads[name].wait()
    attended = acc[...].astype(jnp.bfloat16)
    for start in range(0, model, 512):
        pbuf[:, start : start + 512] = contract(
            attended, ow_ref[:, start : start + 512], (1, 0)
        ).astype(jnp.bfloat16)

    def own_rows(index):
        return pl.ds(pl.multiple_of(index * quarter, quarter), quarter)

    r_copies = []
    for step in range(1, tp_count):
        dest = tp_peer(step)
        r_copies.append(
            launch(pbuf.at[own_rows(dest)], rbuf.at[step - 1], r_sems, (step - 1,), (g, s, dest))
        )
    mixed = pbuf[own_rows(t), :].astype(jnp.float32)
    for index, made in enumerate(r_copies):
        made.wait_recv()
        mixed = mixed + rbuf[index].astype(jnp.float32)
    middle[...] = (res_ref[...].astype(jnp.float32) + mixed).astype(jnp.bfloat16)
    wide = middle[...].astype(jnp.float32)
    mean_square = jnp.mean(wide * wide, axis=1, keepdims=True)
    n_all[s, t] = (
        wide * lax.rsqrt(mean_square + norm_eps) * gain_ref[...].astype(jnp.float32).reshape(1, model)
    ).astype(jnp.bfloat16)

    up, down = 0, 1
    slots = [(step, way) for step in range(1, sp_count) for way in (up, down)]

    def place_of(origin, step, way):
        return origin - step if way == up else origin + step

    def inside(place):
        return (place >= 0) & (place < sp_count)

    def wrap(place):
        return lax.rem(place + 2 * sp_count, sp_count)

    def chain_copy(view, sems, way, hop, index):
        onward = wrap(s + 1 if way == up else s - 1)
        return copy(view, view, sems, (way, hop) + index, (g, onward, t))

    def chain_start(view, sems, way, hop, index, valid):
        going = valid & inside(s + 1 if way == up else s - 1)
        made = chain_copy(view, sems, way, hop, index)
        pl.when(going)(made.start)
        guarded.append((going, made))

    def spread(ref, sems, index, valid):
        first = (
            copy(ref(t), ref(t), sems, (0, index), (g, s, far_mate)),
            copy(ref(t), ref(t), sems, (1, index), (g, s, core_mate)),
        )
        for made in first:
            pl.when(valid)(made.start)
            guarded.append((valid, made))
        return first

    def finish(ref, sems, index, first, valid):
        relayed = copy(ref(far_mate), ref(far_mate), sems, (2, index), (g, s, core_mate))

        @pl.when(valid)
        def _():
            first[0].wait_recv()
            relayed.start()
            first[1].wait_recv()
            relayed.wait_recv()

        guarded.append((valid, relayed))

    def n_view(block):
        return lambda place: n_all.at[block, place]

    def slot_number(slot):
        return 0 if slot is None else 1 + slots.index(slot)

    always = s >= 0
    spreads = {}

    def arrive(slot):
        step, way = slot
        origin = place_of(s, step, way)
        valid, block = inside(origin), wrap(origin)
        view = n_all.at[block, t]
        pl.when(valid)(chain_copy(view, n_sems, way, step - 1, ()).wait_recv)
        if step < sp_count - 1:
            chain_start(view, n_sems, way, step, (), valid)
        spreads[slot] = spread(n_view(block), f_sems, slot_number(slot), valid)

    def process(slot):
        origin = s if slot is None else place_of(s, *slot)
        valid = always if slot is None else inside(origin)
        block = wrap(origin)
        number = slot_number(slot)
        finish(n_view(block), f_sems, number, spreads[slot], valid)

        @pl.when(valid)
        def _():
            total = jnp.zeros((2 * piece, rows), jnp.float32)
            tokens = n_all[block].reshape(rows, model)
            for part in range(sp_count):
                total = total + contract(
                    w_all[part].reshape(2 * piece, slab),
                    tokens[:, part * slab : (part + 1) * slab],
                    (1, 1),
                )
            gate_pre, up_pre = total[:piece], total[piece:]
            h_all[block, s] = (gate_pre / (1.0 + jnp.exp(-gate_pre)) * up_pre).astype(jnp.bfloat16)

        for way in (up, down):
            chain_start(h_all.at[block, s], h_sems, way, 0, (number,), valid)

    def hop_on(slot, step, way):
        if slot is not None and slot[1] == way and slot[0] + step >= sp_count:
            return
        source = place_of(s, step, way)
        target = source if slot is None else place_of(source, *slot)
        valid = inside(source) & inside(target)
        view, index = h_all.at[wrap(target), wrap(source)], (slot_number(slot),)
        pl.when(valid)(chain_copy(view, h_sems, way, step - 1, index).wait_recv)
        if step < sp_count - 1:
            chain_start(view, h_sems, way, step, index, valid)

    def hop_all(stage):
        for distance in range(stage):
            step = stage - distance
            if step < sp_count and distance < sp_count:
                for slot in [None] if distance == 0 else [(distance, up), (distance, down)]:
                    for way in (up, down):
                        hop_on(slot, step, way)

    for way in (up, down):
        chain_start(n_all.at[s, t], n_sems, way, 0, (), always)
    spreads[None] = spread(n_view(s), f_sems, 0, always)
    y_copies = []
    for step in range(1, sp_count):
        w_copies[step].wait_recv()
        view = w_all.at[sp_peer(-step), g]
        y_copies.append(launch(view, view, wy_sems, (step - 1,), (1 - g, s, t)))
    arrive((1, up))
    arrive((1, down))
    for made in y_copies:
        made.wait_recv()
    process(None)
    for stage in range(1, sp_count):
        for way in (up, down):
            if stage < sp_count - 1:
                arrive((stage + 1, way))
        for way in (up, down):
            process((stage, way))
        hop_all(stage)
    for stage in range(sp_count, 2 * sp_count - 1):
        hop_all(stage)

    d_copies = {}
    order = list(range(1, sp_count)) + [0]
    for step in order:
        block = sp_peer(-step)
        hidden = h_all[block].reshape(sp_count * piece, rows)
        dbuf[block] = contract(hidden, down_ref[...], (0, 0)).astype(jnp.bfloat16)
        for hop, share in enumerate((lax.rem(core_mate + 2, 4), core_mate)):
            d_copies[step, hop] = launch(
                dbuf.at[block, own_rows(share)],
                rdown.at[hop, step],
                d_sems,
                (step, hop),
                (g, s, core_mate),
            )
    for step in order:
        d_copies[step, 0].wait_recv()
        pair = dbuf[sp_peer(-step), own_rows(far_mate), :].astype(jnp.float32)
        psend[step] = (pair + rdown[0, step].astype(jnp.float32)).astype(jnp.bfloat16)
        d_copies[step, 2] = launch(
            psend.at[step], rdown.at[2, step], d_sems, (step, 2), (g, s, far_mate)
        )
    z_copies = {}
    for step in order:
        block = sp_peer(-step)
        summed = dbuf[block, own_rows(t), :].astype(jnp.float32)
        for hop in (1, 2):
            d_copies[step, hop].wait_recv()
            summed = summed + rdown[hop, step].astype(jnp.float32)
        if step:
            zsend[step - 1] = summed.astype(jnp.bfloat16)
            z_copies[step] = launch(
                zsend.at[step - 1], zin.at[s], z_sems, (step - 1,), (g, block, t)
            )
        else:
            zin[s] = summed.astype(jnp.bfloat16)
    for step in range(1, sp_count):
        z_copies[step].wait_recv()
    for part in range(sp_count):
        cols = slice(part * slab, (part + 1) * slab)
        out_ref[own_rows(t), cols] = (
            middle[:, cols].astype(jnp.float32) + zin[part].astype(jnp.float32)
        ).astype(jnp.bfloat16)

    def out_view(place):
        return out_ref.at[own_rows(place)]

    finish(out_view, o_sems, 0, spread(out_view, o_sems, 0, always), always)
    for made in sends:
        made.wait_send()
    for valid, made in guarded:
        pl.when(valid)(made.wait_send)
    for step in range(1, sp_count):

        @pl.when(s + step < sp_count)
        def _():
            for made in kv_copies[step]:
                made.wait_send()


def fused_body(
    grp_count,
    sp_count,
    tp_count,
    queries,
    key_rows,
    value_rows,
    key_bias,
    residual,
    out_weight,
    norm_gain,
    gate_weight,
    up_weight,
    down_weight,
):
    rows, columns = queries.shape
    head_count = key_bias.shape[0]
    model = residual.shape[1]
    hidden = gate_weight.shape[1]
    piece, slab, quarter = hidden // sp_count, model // sp_count, rows // tp_count
    n, m = sp_count - 1, tp_count - 1
    half, wide = jnp.bfloat16, jnp.float32
    dma = pltpu.SemaphoreType.DMA
    return pl.pallas_call(
        functools.partial(layer_kernel, grp_count, sp_count, tp_count),
        out_shape=jax.ShapeDtypeStruct((rows, model), half),
        in_specs=[pl.BlockSpec(memory_space=pl.ANY)] * 10,
        out_specs=pl.BlockSpec(memory_space=pltpu.VMEM),
        scratch_shapes=[
            pltpu.VMEM((rows, columns), half),
            pltpu.VMEM((rows, columns), half),
            pltpu.VMEM((rows, columns), half),
            pltpu.VMEM((head_count, rows), half),
            pltpu.VMEM((quarter, model), half),
            pltpu.VMEM((columns, model), half),
            pltpu.VMEM((model,), half),
            pltpu.VMEM((slab, hidden), half),
            pltpu.VMEM((slab, hidden), half),
            pltpu.VMEM((hidden, slab), half),
            dma((10,)),
            pltpu.VMEM((n, rows, columns), half),
            pltpu.VMEM((n, rows, columns), half),
            pltpu.VMEM((n, head_count, rows), half),
            pltpu.VMEM((rows, columns), wide),
            pltpu.VMEM((head_count, rows, 1), wide),
            pltpu.VMEM((2, hidden, slab), half),
            pltpu.VMEM((sp_count, 2, piece, slab), half),
            pltpu.VMEM((rows, model), half),
            pltpu.VMEM((m, quarter, model), half),
            pltpu.VMEM((quarter, model), half),
            pltpu.VMEM((sp_count, tp_count, quarter, model), half),
            pltpu.VMEM((sp_count, sp_count, piece, rows), half),
            pltpu.VMEM((sp_count, rows, slab), half),
            pltpu.VMEM((m, sp_count, quarter, slab), half),
            pltpu.VMEM((sp_count, quarter, slab), half),
            pltpu.VMEM((n, quarter, slab), half),
            pltpu.VMEM((sp_count, quarter, slab), half),
            dma((2, 3, n)),
            dma((2, n)),
            dma((2, n)),
            dma((2, m)),
            dma((2, 2, n)),
            dma((2, 3, 2 * n + 1)),
            dma((2, 2, n, 2 * n + 1)),
            dma((2, sp_count, m)),
            dma((2, n)),
            dma((2, 3, 1)),
        ],
        compiler_params=pltpu.CompilerParams(
            collective_id=0, has_side_effects=True, vmem_limit_bytes=67_043_328
        ),
    )(
        queries,
        key_rows,
        value_rows,
        key_bias,
        residual,
        out_weight,
        norm_gain,
        gate_weight,
        up_weight,
        down_weight,
    )


def any_body(sizes, *arguments):
    grp_count, sp_count, tp_count = sizes
    queries, model, hidden = arguments[0], arguments[4].shape[1], arguments[7].shape[1]
    rows = queries.shape[0]
    fits = (
        grp_count == 2
        and tp_count == 4
        and 1 < sp_count <= 4
        and rows == 128
        and queries.shape[1] == 128
        and (model // sp_count) % 128 == 0
        and (hidden // sp_count) % 16 == 0
        and hidden % 128 == 0
    )
    if fits:
        return fused_body(grp_count, sp_count, tp_count, *arguments)
    return body(*arguments)


def solution(mesh):
    in_specs = (
        P(("grp", "sp"), "tp"),
        P(("grp", "sp"), "tp"),
        P(("grp", "sp"), "tp"),
        P("tp", ("grp", "sp")),
        P(("grp", "sp"), None),
        P("tp", None),
        P(),
        P("sp", "tp"),
        P("sp", "tp"),
        P("tp", "sp"),
    )
    out_specs = P(("grp", "sp"), None)
    sizes = tuple(mesh.shape[name] for name in ("grp", "sp", "tp"))
    return jax.shard_map(functools.partial(any_body, sizes), mesh=mesh, in_specs=in_specs, out_specs=out_specs, check_vma=False)
```
